32 devices in a mesh: rep: 2 (over y), fs: 4 (over z), tp: 4 (over x, core).
Axes of the slice: x: 2, y: 2, z: 4, core: 2. Of those that a mesh axis runs over, the one named last changes fastest.
Arguments:
- activations: bfloat16 [8, 256, 2048], P(('rep', 'fs'), None, 'tp'), may hold values from -15 to 15
- norm_gain: float32 [2048], replicated, may hold values from 0.1 to 1.9
- w_value: bfloat16 [2048, 2048], P('fs', 'tp'), may hold values from -0.125 to 0.125
- w_gate_conv: bfloat16 [2048, 2048], P('fs', 'tp'), may hold values from -0.125 to 0.125
- conv_weight: float32 [31, 2048], P(None, 'tp'), may hold values from -3 to 3
- chan_gain: float32 [2048], P('tp'), may hold values from 0.1 to 1.9
- w_conv_out: bfloat16 [2048, 2048], P('tp', 'fs'), may hold values from -0.125 to 0.125
- mix_gain: float32 [2048], replicated, may hold values from 0.1 to 1.9
- w_gate: bfloat16 [2048, 3072], P('fs', 'tp'), may hold values from -0.125 to 0.125
- w_up: bfloat16 [2048, 3072], P('fs', 'tp'), may hold values from -0.125 to 0.125
- w_down: bfloat16 [3072, 2048], P('tp', 'fs'), may hold values from -0.109375 to 0.109375
- final_gain: float32 [2048], P('tp'), may hold values from 0.1 to 1.9
Outputs:
- result: bfloat16 [8, 256, 2048], P(('rep', 'fs'), None, 'tp')
The draws below stay inside these ranges and needn't reach their ends.
All inputs are finite; a program needn't handle non-finite values.
Results may differ from the reference program's by a relative error of at most 0.013.
Values may be sent and summed in bfloat16 or wider, within the bound.
No kernel may reach another device: no remote copies, remote signals or barrier semaphores. Data moves between devices by JAX's collectives and lax.ppermute only.
A program may use at most 64 MiB of HBM per device.

```python
import jax
import jax.numpy as jnp
from jax import lax

D = 2048
C = 2048
FF = 3072
K = 31
SEQ = 256
BATCH = 8
N_TP = 4


def draw_activations(key, part):
    column = jnp.arange(D, dtype=jnp.float32)
    scale = 0.3 * 10.0 ** (column / (D - 1))
    values = jax.random.normal(key, (BATCH, SEQ, D), jnp.float32) * scale
    return jnp.clip(values, -15.0, 15.0).astype(jnp.bfloat16)


def draw_conv_weight(key, part):
    channel = jnp.arange(C, dtype=jnp.float32)
    scale = 0.35 * 8.0 ** (channel / (C - 1)) / jnp.sqrt(jnp.float32(K))
    values = jnp.clip(jax.random.normal(key, (K, C), jnp.float32), -4.0, 4.0) * scale
    return jnp.clip(values, -3.0, 3.0).astype(jnp.float32)


def levels(key, extent, cuts, least, largest):
    level, own = 1.0, jax.random.fold_in(key, 6)
    for dim, blocks in cuts:
        heights = jnp.exp(jax.random.uniform(jax.random.fold_in(own, dim), (blocks,), jnp.float32, least / len(cuts), largest / len(cuts)))
        level = level * jnp.repeat(heights, extent[dim] // blocks).reshape([-1 if axis == dim else 1 for axis in range(len(extent))])
    return level


def centred(key, shape, scale, limit, pieces=(), kind=jnp.bfloat16):
    array = scale * jax.random.normal(key, shape, jnp.float32)
    if pieces:
        array = array * levels(key, shape, pieces, -0.22, 0.18)
    return jnp.clip(array, -limit, limit).astype(kind)


def setup_inputs(seed: int = 0) -> dict:
    keys = jax.random.split(jax.random.key(seed), 13)
    activations = draw_activations(jax.random.fold_in(keys[12], 71), 0)
    norm_gain = jnp.clip(1.0 + 0.18 * jax.random.normal(keys[1], (D,), jnp.float32), 0.1, 1.9)
    w_value = centred(keys[2], (D, C), D ** -0.5, 0.125, ((0, 4), (1, 4)))
    w_gate_conv = centred(keys[3], (D, C), D ** -0.5, 0.125, ((0, 4), (1, 4)))
    conv_weight = draw_conv_weight(jax.random.fold_in(keys[12], 71), 0)
    chan_gain = jnp.clip(1.0 + 0.18 * jax.random.normal(keys[5], (C,), jnp.float32), 0.1, 1.9)
    w_conv_out = centred(keys[6], (C, D), C ** -0.5, 0.125, ((0, 4), (1, 4)))
    mix_gain = jnp.clip(1.0 + 0.18 * jax.random.normal(keys[7], (D,), jnp.float32), 0.1, 1.9)
    w_gate = centred(keys[8], (D, FF), D ** -0.5, 0.125, ((0, 4), (1, 4)))
    w_up = centred(keys[9], (D, FF), D ** -0.5, 0.125, ((0, 4), (1, 4)))
    w_down = centred(keys[10], (FF, D), FF ** -0.5, 0.109375, ((0, 4), (1, 4)))
    final_gain = jnp.clip(1.0 + 0.18 * jax.random.normal(keys[11], (D,), jnp.float32), 0.1, 1.9)
    return {"activations": activations, "norm_gain": norm_gain, "w_value": w_value, "w_gate_conv": w_gate_conv, "conv_weight": conv_weight, "chan_gain": chan_gain, "w_conv_out": w_conv_out, "mix_gain": mix_gain, "w_gate": w_gate, "w_up": w_up, "w_down": w_down, "final_gain": final_gain}


EPS = 1e-06

def rms_scale(values, gain):
    return values * lax.rsqrt(lax.optimization_barrier(jnp.mean(values * values, axis=-1, keepdims=True)) + EPS) * gain

def blocked_product(left, weight):
    span = weight.shape[0] // N_TP
    total = jnp.zeros((left.shape[0], weight.shape[1]), jnp.float32)
    for block in range(N_TP):
        part = jnp.dot(left[:, block * span:(block + 1) * span], weight[block * span:(block + 1) * span], preferred_element_type=jnp.float32).astype(jnp.bfloat16)
        part = lax.optimization_barrier(part)
        total = total + part.astype(jnp.float32)
    return total

def reference(activations, norm_gain, w_value, w_gate_conv, conv_weight, chan_gain, w_conv_out, mix_gain, w_gate, w_up, w_down, final_gain):

    def one_sequence(sequence):
        residual = sequence.astype(jnp.float32)
        normed_in = rms_scale(residual, norm_gain).astype(jnp.bfloat16)
        value = jnp.dot(normed_in, w_value, preferred_element_type=jnp.float32)
        gate_conv = jnp.dot(normed_in, w_gate_conv, preferred_element_type=jnp.float32)
        glu = value * jax.nn.sigmoid(gate_conv)
        padded = jnp.pad(glu, ((K - 1, 0), (0, 0)))
        conv = jnp.zeros_like(glu)
        for tap in range(K):
            conv = conv + conv_weight[tap][None, :] * padded[tap:tap + SEQ]
        mean = lax.optimization_barrier(jnp.mean(conv, axis=-1, keepdims=True))
        centered = conv - mean
        spread = lax.optimization_barrier(jnp.mean(centered * centered, axis=-1, keepdims=True))
        act = jax.nn.silu(centered * lax.rsqrt(spread + EPS) * chan_gain).astype(jnp.bfloat16)
        first = (residual + blocked_product(act, w_conv_out)).astype(jnp.bfloat16)
        first_f = first.astype(jnp.float32)
        normed_mid = rms_scale(first_f, mix_gain).astype(jnp.bfloat16)
        gate = jnp.dot(normed_mid, w_gate, preferred_element_type=jnp.float32)
        up = jnp.dot(normed_mid, w_up, preferred_element_type=jnp.float32)
        hidden = (jax.nn.silu(gate) * up).astype(jnp.bfloat16)
        second = first_f + blocked_product(hidden, w_down)
        return rms_scale(second, final_gain).astype(jnp.bfloat16)
    return lax.map(one_sequence, activations)
```

```python
import functools

import jax
import jax.numpy as jnp
from jax import lax
from jax.experimental import pallas as pl
from jax.experimental.pallas import tpu as pltpu
from jax.sharding import PartitionSpec as P

EPS = 1e-06
AXES = ("rep", "fs", "tp")
F32 = jnp.float32
BF16 = jnp.bfloat16


def plain_body(
    activations,
    norm_gain,
    w_value,
    w_gate_conv,
    conv_weight,
    chan_gain,
    w_conv_out,
    mix_gain,
    w_gate,
    w_up,
    w_down,
    final_gain,
):
    batch, length, local_width = activations.shape
    width = local_width * lax.axis_size("tp")
    count = batch * length
    residual = activations.reshape(count, local_width).astype(F32)
    raw_in = lax.all_gather(
        activations.reshape(count, local_width), "tp", axis=1, tiled=True
    ).astype(F32)
    in_mean = jnp.mean(raw_in * raw_in, axis=1, keepdims=True)
    rows_in = (raw_in * lax.rsqrt(in_mean + EPS) * norm_gain).astype(BF16)
    chan_local = w_value.shape[1]
    value = jnp.dot(
        rows_in, lax.all_gather(w_value, "fs", axis=0, tiled=True), preferred_element_type=F32
    )
    gate_conv = jnp.dot(
        rows_in, lax.all_gather(w_gate_conv, "fs", axis=0, tiled=True), preferred_element_type=F32
    )
    glu = (value * jax.nn.sigmoid(gate_conv)).reshape(batch, length, chan_local)
    taps = conv_weight.shape[0]
    padded = jnp.pad(glu, ((0, 0), (taps - 1, 0), (0, 0)))
    conv = lax.conv_general_dilated(
        padded,
        conv_weight[:, None, :],
        (1,),
        "VALID",
        dimension_numbers=("NWC", "WIO", "NWC"),
        feature_group_count=chan_local,
        precision=lax.Precision.HIGHEST,
    ).reshape(count, chan_local)
    chan_total = chan_local * lax.axis_size("tp")
    mean = lax.psum(jnp.sum(conv, axis=1), "tp") / chan_total
    centered = conv - mean[:, None]
    spread = lax.psum(jnp.sum(centered * centered, axis=1), "tp") / chan_total
    act = jax.nn.silu(centered * lax.rsqrt(spread + EPS)[:, None] * chan_gain).astype(BF16)
    conv_terms = jnp.dot(
        act, lax.all_gather(w_conv_out, "fs", axis=1, tiled=True), preferred_element_type=F32
    )
    conv_out = lax.psum_scatter(
        conv_terms.astype(BF16), "tp", scatter_dimension=1, tiled=True
    ).astype(F32)
    first = (residual + conv_out).astype(BF16)
    raw_mid = lax.all_gather(first, "tp", axis=1, tiled=True).astype(F32)
    mid_mean = jnp.mean(raw_mid * raw_mid, axis=1, keepdims=True)
    rows_mid = (raw_mid * lax.rsqrt(mid_mean + EPS) * mix_gain).astype(BF16)
    gate = jnp.dot(
        rows_mid, lax.all_gather(w_gate, "fs", axis=0, tiled=True), preferred_element_type=F32
    )
    up = jnp.dot(
        rows_mid, lax.all_gather(w_up, "fs", axis=0, tiled=True), preferred_element_type=F32
    )
    hidden = (jax.nn.silu(gate) * up).astype(BF16)
    ff_terms = jnp.dot(
        hidden, lax.all_gather(w_down, "fs", axis=1, tiled=True), preferred_element_type=F32
    )
    ff_out = lax.psum_scatter(
        ff_terms.astype(BF16), "tp", scatter_dimension=1, tiled=True
    ).astype(F32)
    second = first.astype(F32) + ff_out
    out_total = lax.psum(jnp.sum(second * second, axis=1), "tp")
    result = (second * lax.rsqrt(out_total / width + EPS)[:, None] * final_gain).astype(BF16)
    return result.reshape(batch, length, local_width)


def permute(x, pairs, name):
    with jax.named_scope(name):
        return lax.ppermute(x, AXES, pairs)


def send(sizes, move):
    reps, spans, parts = sizes
    pairs = []
    for r in range(reps):
        for f in range(spans):
            for t in range(parts):
                to = move(r, f, t)
                if to is not None:
                    pairs.append(((r * spans + f) * parts + t, (to[0] * spans + to[1]) * parts + to[2]))
    return tuple(pairs)


VMEM = pl.BlockSpec(memory_space=pltpu.VMEM)
SMEM = pl.BlockSpec(memory_space=pltpu.SMEM)


def norm_kernel(idx, *refs):
    blocks, gain, out = refs[:-2], refs[-2], refs[-1]
    r, t = idx[0], idx[2]
    parts = len(blocks) // 2
    rows, span = blocks[0].shape
    for q in range(2):
        total = jnp.zeros((rows, 1), F32)
        for m in range(parts):
            b = blocks[q * parts + m][...].astype(F32)
            total = total + jnp.sum(b * b, axis=1, keepdims=True)
        scale = lax.rsqrt(total / (parts * span) + EPS)
        for m in range(parts):
            k = t ^ m
            b = blocks[q * parts + m][...].astype(F32)
            out[k, pl.ds((r ^ q) * rows, rows), :] = (b * scale * gain[k]).astype(BF16)


def pick_last(idx, near, far, buf):
    @pl.when(idx[3] == 1)
    def _():
        buf[...] = near[...]

    @pl.when(idx[3] == 0)
    def _():
        buf[...] = far[...]


def glu_kernel(idx, normed, w0, w1, w2, near, far, taps, conv, stats, buf, padded, cols):
    f = idx[1]
    pick_last(idx, near, far, buf)
    rows = normed.shape[1]
    chans = w0.shape[1] // 2
    lanes = padded.shape[-1]
    seqs, held = padded.shape[1], padded.shape[2]
    length = rows // seqs
    lead = held - length
    n_taps = taps.shape[0]
    half = chans // lanes
    slots = (w0, w1, w2, buf)
    for q in range(seqs):
        span = pl.ds(q * length, length)
        value = jnp.zeros((length, chans), F32)
        gate = jnp.zeros((length, chans), F32)
        for s, w in enumerate(slots):
            x = normed[f ^ s, span, :]
            value = value + jnp.dot(x, w[:, :chans], preferred_element_type=F32)
            gate = gate + jnp.dot(x, w[:, chans:], preferred_element_type=F32)
        glu = value * jax.nn.sigmoid(gate)
        for h in range(half):
            padded[h, q, :lead, :] = jnp.zeros((lead, lanes), F32)
            padded[h, q, lead:, :] = glu[:, h * lanes:(h + 1) * lanes]
    step = 64
    lane = lax.broadcasted_iota(jnp.int32, (step, lanes), 1)

    for q in range(seqs):
        def chunk(i, carry, q=q):
            base = pl.multiple_of(i * step, step)
            outs = []
            for h in range(half):
                acc = jnp.zeros((step, lanes), F32)
                for j in range(n_taps):
                    tap = taps[j:j + 1, h * lanes:(h + 1) * lanes]
                    acc = acc + tap * padded[h, q, pl.ds(base + (lead - n_taps + 1 + j), step), :]
                outs.append(acc)
            total = sum(jnp.sum(o, axis=1, keepdims=True) for o in outs)
            mean = total / chans
            spread = sum(jnp.sum((o - mean) * (o - mean), axis=1, keepdims=True) for o in outs)
            at = pl.ds(q * length + base, step)
            for h in range(half):
                conv[at, h * lanes:(h + 1) * lanes] = outs[h]
            cols[at, :] = jnp.where(lane == 0, mean, jnp.where(lane == 1, spread, 0.0))
            return carry

        lax.fori_loop(0, length // step, chunk, 0)
    for i in range(rows // lanes):
        stats[:, i * lanes:(i + 1) * lanes] = cols[i * lanes:(i + 1) * lanes, :].T[:stats.shape[0], :]


def project(idx, left, slots, keep, give):
    r, f, t = idx[0], idx[1], idx[2]
    rows = left.shape[0] // 2
    for s, w in enumerate(slots):
        m = t ^ f ^ s
        for q in range(2):
            part = jnp.dot(
                left[pl.ds((r ^ q) * rows, rows), :], w[...], preferred_element_type=F32
            ).astype(BF16)

            @pl.when(m % 2 == 0)
            def _(part=part, q=q, m=m):
                keep[m // 2, q] = part

            @pl.when(m % 2 == 1)
            def _(part=part, q=q, m=m):
                give[m // 2, q] = part


def out_kernel(idx, conv, s0, s1, s2, s3, gain, w0, w1, w2, near, far, keep, give, buf, act):
    pick_last(idx, near, far, buf)
    stats = [s[...] for s in (s0, s1, s2, s3)]
    count = 2 * conv.shape[1]
    means = [s[0:1, :] for s in stats]
    mean = sum(means) / len(means)
    spread = sum(s[1:2, :] for s in stats)
    spread = spread + count * sum((m - mean) * (m - mean) for m in means)
    scale = lax.rsqrt(spread / (count * len(stats)) + EPS)
    row = lax.broadcasted_iota(jnp.int32, stats[0].shape, 0)
    both = jnp.where(row == 0, mean, scale)
    side = both.T
    centered = (conv[...] - side[:, 0:1]) * side[:, 1:2] * gain[...]
    act[...] = (centered / (1.0 + jnp.exp(-centered))).astype(BF16)
    project(idx, act, (w0, w1, w2, buf), keep, give)


def hidden_kernel(idx, normed, w0, w1, w2, near, far, hidden, buf):
    f = idx[1]
    pick_last(idx, near, far, buf)
    rows = normed.shape[1] // 2
    units = hidden.shape[1]
    for q in range(2):
        span = pl.ds(q * rows, rows)
        gate = jnp.zeros((rows, units), F32)
        up = jnp.zeros((rows, units), F32)
        for s, w in enumerate((w0, w1, w2, buf)):
            x = normed[f ^ s, span, :]
            gate = gate + jnp.dot(x, w[:, :units], preferred_element_type=F32)
            up = up + jnp.dot(x, w[:, units:], preferred_element_type=F32)
        hidden[span, :] = (gate / (1.0 + jnp.exp(-gate)) * up).astype(BF16)


def down_kernel(idx, hidden, w0, w1, w2, near, far, keep, give, buf):
    pick_last(idx, near, far, buf)
    project(idx, hidden, (w0, w1, w2, buf), keep, give)


def call(kernel, outs, scratch, idx, *args):
    return pl.pallas_call(
        kernel,
        out_shape=outs,
        in_specs=[SMEM] + [VMEM] * len(args),
        out_specs=jax.tree.map(lambda _: VMEM, outs),
        scratch_shapes=scratch,
    )(idx, *args)


def fast_body(
    sizes,
    activations,
    norm_gain,
    w_value,
    w_gate_conv,
    conv_weight,
    chan_gain,
    w_conv_out,
    mix_gain,
    w_gate,
    w_up,
    w_down,
    final_gain,
):
    reps, spans, parts = sizes
    batch, length, span = activations.shape
    count = batch * length
    width = span * parts
    rows = count * reps
    r, f, t = (lax.axis_index(a) for a in AXES)
    mid = ((f > 0) & (f < spans - 1)).astype(jnp.int32)
    idx = jnp.stack([r, f, t, mid]).astype(jnp.int32)

    hop = functools.partial(send, sizes)
    to_core = hop(lambda a, b, c: (a, b, c ^ 1))
    to_x = hop(lambda a, b, c: (a, b, c ^ 2))
    to_y = hop(lambda a, b, c: (a ^ 1, b, c))
    to_xy = hop(lambda a, b, c: (a ^ 1, b, c ^ 2))
    z1 = hop(lambda a, b, c: (a, b ^ 1, c))
    z2 = hop(lambda a, b, c: (a, b ^ 2, c))
    zn = hop(lambda a, b, c: (a, b ^ 3, c) if 0 < b < spans - 1 else None)
    zf = hop(lambda a, b, c: (a, b ^ 1, c) if 0 < b < spans - 1 else None)

    def gather_plane(x, name):
        across = [x] + [permute(x, p, f"{name}{i}") for i, p in enumerate((to_x, to_y, to_xy))]
        beside = [permute(a, to_core, f"{name}c{i}") for i, a in enumerate(across)]
        return [across[0], beside[0], across[1], beside[1], across[2], beside[2], across[3], beside[3]]

    def gather_line(w, name):
        b = permute(w, z2, f"{name}b")
        a = permute(w, z1, f"{name}a")
        near = permute(w, zn, f"{name}n")
        far = permute(b, zf, f"{name}f")
        return w, a, b, near, far

    def reduce_plane(keep, give, name):
        got = permute(give, to_core, f"{name}c")
        both = keep.astype(F32) + got.astype(F32)
        mine = both[0, 0]
        parts_ = (
            permute(both[1, 0].astype(BF16), to_x, f"{name}0"),
            permute(both[0, 1].astype(BF16), to_y, f"{name}1"),
            permute(both[1, 1].astype(BF16), to_xy, f"{name}2"),
        )
        return mine + sum(p.astype(F32) for p in parts_)

    def columns(w):
        own = w.shape[1] // reps
        return lax.dynamic_slice_in_dim(w, r * own, own, axis=1)

    def lines(w):
        own = w.shape[0] // reps
        return lax.dynamic_slice_in_dim(w, r * own, own, axis=0)

    x = activations.reshape(count, span)
    xs = gather_plane(x, "px")
    g1 = gather_line(jnp.concatenate([columns(w_value), columns(w_gate_conv)], axis=1), "g1")
    g2 = gather_line(lines(w_conv_out), "g2")
    g3 = gather_line(jnp.concatenate([columns(w_gate), columns(w_up)], axis=1), "g3")
    g4 = gather_line(lines(w_down), "g4")

    def norm(blocks, gain):
        return call(
            norm_kernel,
            jax.ShapeDtypeStruct((parts, rows, span), BF16),
            [],
            idx,
            *blocks,
            gain.reshape(parts, 1, span),
        )

    normed_in = norm(xs, norm_gain)
    chans = g1[0].shape[1] // 2
    taps = columns(conv_weight)
    lanes = 128
    lead = -(-(taps.shape[0] - 1) // 8) * 8
    conv, stats = call(
        glu_kernel,
        (jax.ShapeDtypeStruct((rows, chans), F32), jax.ShapeDtypeStruct((8, rows), F32)),
        [
            pltpu.VMEM(g1[0].shape, BF16),
            pltpu.VMEM((chans // lanes, reps, lead + count, lanes), F32),
            pltpu.VMEM((rows, lanes), F32),
        ],
        idx,
        normed_in,
        *g1,
        taps,
    )
    other = permute(stats, to_core, "psc")
    apart = stats[0:1] - other[0:1]
    pair = jnp.concatenate(
        [
            0.5 * (stats[0:1] + other[0:1]),
            stats[1:2] + other[1:2] + apart * apart * (0.5 * chans),
            jnp.zeros_like(stats[2:]),
        ],
        axis=0,
    )
    moments = [pair] + [permute(pair, p, f"ps{i}") for i, p in enumerate((to_x, to_y, to_xy))]
    halves = (jax.ShapeDtypeStruct((parts // 2, reps, count, span), BF16),) * 2
    keep, give = call(
        out_kernel,
        halves,
        [pltpu.VMEM(g2[0].shape, BF16), pltpu.VMEM((rows, chans), BF16)],
        idx,
        conv,
        *moments,
        lax.dynamic_slice_in_dim(chan_gain, r * chans, chans).reshape(1, chans),
        *g2,
    )
    conv_out = reduce_plane(keep, give, "pr")
    first = (x.astype(F32) + conv_out).astype(BF16)
    normed_mid = norm(gather_plane(first, "pm"), mix_gain)
    units = g3[0].shape[1] // 2
    hidden = call(
        hidden_kernel,
        jax.ShapeDtypeStruct((rows, units), BF16),
        [pltpu.VMEM(g3[0].shape, BF16)],
        idx,
        normed_mid,
        *g3,
    )
    keep, give = call(down_kernel, halves, [pltpu.VMEM(g4[0].shape, BF16)], idx, hidden, *g4)
    second = first.astype(F32) + reduce_plane(keep, give, "pd")
    total = jnp.sum(second * second, axis=1)
    total = total + permute(total, to_core, "pec")
    total = total + permute(total, to_x, "pex")
    result = (second * lax.rsqrt(total / width + EPS)[:, None] * final_gain).astype(BF16)
    return result.reshape(batch, length, span)


def solution(mesh):
    in_specs = (
        P(("rep", "fs"), None, "tp"),
        P(),
        P("fs", "tp"),
        P("fs", "tp"),
        P(None, "tp"),
        P("tp"),
        P("tp", "fs"),
        P(),
        P("fs", "tp"),
        P("fs", "tp"),
        P("tp", "fs"),
        P("tp"),
    )
    out_specs = P(("rep", "fs"), None, "tp")
    sizes = tuple(mesh.shape[a] for a in AXES)
    pair, line = 2, 4
    if sizes == (pair, line, line):
        body = functools.partial(fast_body, sizes)
    else:
        body = plain_body
    return jax.shard_map(body, mesh=mesh, in_specs=in_specs, out_specs=out_specs, check_vma=False)
```
